32 devices in a mesh: sp: 8 (over z, core), tp: 4 (over y, x).
Axes of the slice: x: 2, y: 2, z: 4, core: 2. Of those that a mesh axis runs over, the one named last changes fastest.
Arguments:
- stream: bfloat16 [1024, 2048], P('sp'), may hold values from -6 to 6
- query_small: bfloat16 [1024, 1024], P('sp', 'tp'), may hold values from -6 to 6
- key_small: bfloat16 [1024, 1024], P('sp', 'tp'), may hold values from -6 to 6
- value_small: bfloat16 [1024, 1024], P('sp', 'tp'), may hold values from -6 to 6
- query_large: bfloat16 [1024, 2048], P('sp', 'tp'), may hold values from -6 to 6
- key_large: bfloat16 [1024, 2048], P('sp', 'tp'), may hold values from -6 to 6
- value_large: bfloat16 [1024, 2048], P('sp', 'tp'), may hold values from -6 to 6
- key_bias: bfloat16 [1024, 2, 16], P('sp', None, 'tp'), may hold values from -16 to 1
- out_small: bfloat16 [1024, 2048], P('tp'), may hold values from -0.75 to 0.75
- out_large: bfloat16 [2048, 2048], P('tp'), may hold values from -0.75 to 0.75
- gain_one: float32 [2048], replicated, may hold values from 0.1 to 1.9
- shift_one: float32 [2048], replicated, may hold values from -1.5 to 1.5
- gain_two: float32 [2048], replicated, may hold values from 0.1 to 1.9
- shift_two: float32 [2048], replicated, may hold values from -1.5 to 1.5
- expert_pick: int32 [1024, 2], P('sp'), may hold values from 0 to 7, as said below
- route_weight: float32 [1024, 2], P('sp'), may hold values from 0.2 to 1
- w_gate: bfloat16 [8, 2048, 4096], P('sp', None, 'tp'), may hold values from -0.125 to 0.125
- w_up: bfloat16 [8, 2048, 4096], P('sp', None, 'tp'), may hold values from -0.125 to 0.125
- w_down: bfloat16 [8, 4096, 2048], P('sp', 'tp'), may hold values from -0.09375 to 0.09375
Outputs:
- result: bfloat16 [1024, 2048], P(('sp', 'tp'))
The draws below stay inside these ranges and needn't reach their ends.
Inputs may be any that keep to these rules, and one draw needn't show every extreme that they name: In each aligned block of 128 positions (the positions of one index of sp), no expert is named more than 64 times, and in every block some expert is named exactly 64 times. The two experts of a position differ and lie in one group: equal values of expert_pick // 2.
All inputs are finite; a program needn't handle non-finite values.
Results may differ from the reference program's by a relative error of at most 0.017.
Values may be sent and summed in bfloat16 or wider, within the bound.
A program may use at most 64 MiB of HBM per device.

```python
import jax
import jax.numpy as jnp
from jax import lax

D = 2048
HEADS_PER_GROUP = 16
HEAD_SMALL = 64
HEAD_LARGE = 128
FF_E = 4096
GROUPS = 4
TOK_DEV = 128
SEQUENCE_LENGTH = 1024
EXPERTS = 8
PER_GROUP = 2
CAP = 64
N_TP = 4


def draw_key_bias(key, part):
    key_matrix = jax.random.split(key, 7)
    head_shape = (2, HEADS_PER_GROUP)
    fast_share = 0.5
    slow_low = 1.0
    slow_high = 2.0
    fast_heads = jax.random.uniform(key_matrix[0], head_shape) < fast_share
    slow_rate = jax.random.uniform(key_matrix[1], head_shape, minval=slow_low, maxval=slow_high) / SEQUENCE_LENGTH
    fast_rate = 1.0 / jax.random.uniform(key_matrix[2], head_shape, minval=30.0, maxval=100.0)
    rate = jnp.where(fast_heads, fast_rate, slow_rate)
    block_factor = jnp.exp(jax.random.uniform(key_matrix[3], (SEQUENCE_LENGTH // TOK_DEV, 2, HEADS_PER_GROUP), minval=-0.7, maxval=0.7))
    block_factor = jnp.repeat(block_factor, TOK_DEV, axis=0)
    baseline_logit = jnp.log(rate[None] * block_factor) - 0.5
    spike_mask = jax.random.uniform(key_matrix[4], (SEQUENCE_LENGTH, 2, HEADS_PER_GROUP)) < 2.0 / SEQUENCE_LENGTH
    spike_level = jax.random.uniform(key_matrix[5], (SEQUENCE_LENGTH, 2, HEADS_PER_GROUP), minval=0.2, maxval=0.5)
    spike_logit = jnp.log(spike_level / (1.0 - spike_level))
    perturbation_term = 0.3 * jax.random.normal(key_matrix[6], (SEQUENCE_LENGTH, 2, HEADS_PER_GROUP))
    sampled_values = jnp.where(spike_mask, spike_logit, baseline_logit + perturbation_term)
    return sampled_values.astype(jnp.float32).astype(jnp.bfloat16)


def value_field(key, columns):
    key_matrix = jax.random.split(key, 2)
    sampled_values = jnp.clip(jax.random.normal(key_matrix[1], (SEQUENCE_LENGTH, columns)), -6.0, 6.0)
    return sampled_values.astype(jnp.float32).astype(jnp.bfloat16)


def draw_value_small(key, part):
    return value_field(jax.random.fold_in(key, 101), HEADS_PER_GROUP * HEAD_SMALL)


def draw_value_large(key, part):
    return value_field(jax.random.fold_in(key, 202), HEADS_PER_GROUP * HEAD_LARGE)


def group_cycle(sub_key):
    return jax.random.permutation(sub_key, PER_GROUP).astype(jnp.int32)


def pick_block(key):
    key_matrix = jax.random.split(key, 4)
    order = jnp.argsort(jax.random.permutation(key_matrix[0], TOK_DEV)).astype(jnp.int32)
    group_cap = PER_GROUP * CAP // 2
    group_order = jax.random.permutation(key_matrix[1], GROUPS).astype(jnp.int32)
    cut_pair = jax.random.randint(key_matrix[2], (2,), group_cap, TOK_DEV + 1).astype(jnp.int32)
    cut_low = jnp.min(cut_pair)
    cut_high = jnp.max(cut_pair)
    bucket = (order >= group_cap).astype(jnp.int32) + (order >= cut_low).astype(jnp.int32) + (order >= cut_high).astype(jnp.int32)
    offsets = jnp.stack([jnp.int32(0), jnp.int32(group_cap), cut_low, cut_high])
    in_group = order - offsets[bucket]
    group_id = group_order[bucket]
    cycles = jax.vmap(group_cycle)(jax.random.split(key_matrix[3], GROUPS))
    first_pick = cycles[group_id, 2 * in_group % PER_GROUP]
    second_pick = cycles[group_id, (2 * in_group + 1) % PER_GROUP]
    return jnp.stack([group_id * PER_GROUP + first_pick, group_id * PER_GROUP + second_pick], axis=-1).astype(jnp.int32)


def draw_expert_pick(key, part):
    return jax.vmap(pick_block)(jax.random.split(key, SEQUENCE_LENGTH // TOK_DEV)).reshape(SEQUENCE_LENGTH, 2)


def level_of(key, extent, cuts, smallest, high):
    factor_of, own = 1.0, jax.random.fold_in(key, 6)
    for position, parts in cuts:
        heights = jnp.exp(jax.random.uniform(jax.random.fold_in(own, position), (parts,), jnp.float32, smallest / len(cuts), high / len(cuts)))
        factor_of = factor_of * jnp.repeat(heights, extent[position] // parts).reshape([-1 if axis == position else 1 for axis in range(len(extent))])
    return factor_of


def bell_draw(own_key, dims, scale, bound, cuts=(), held_as=jnp.bfloat16):
    values = scale * jax.random.normal(own_key, dims, jnp.float32)
    if cuts:
        values = values * level_of(own_key, dims, cuts, -0.22, 0.18)
    return jnp.clip(values, -bound, bound).astype(held_as)


def setup_inputs(seed: int = 0) -> dict:
    key_list = jax.random.split(jax.random.key(seed), 20)
    stream = bell_draw(key_list[0], (SEQUENCE_LENGTH, D), 1.0, 6.0, ((0, 8),))
    query_small = bell_draw(key_list[1], (SEQUENCE_LENGTH, HEADS_PER_GROUP * HEAD_SMALL), 1.0, 6.0, ((0, 8), (1, 4)))
    key_small = bell_draw(key_list[2], (SEQUENCE_LENGTH, HEADS_PER_GROUP * HEAD_SMALL), 1.0, 6.0, ((0, 8), (1, 4)))
    value_small = draw_value_small(jax.random.fold_in(key_list[19], 71), 0)
    query_large = bell_draw(key_list[4], (SEQUENCE_LENGTH, HEADS_PER_GROUP * HEAD_LARGE), 1.0, 6.0, ((0, 8), (1, 4)))
    key_large = bell_draw(key_list[5], (SEQUENCE_LENGTH, HEADS_PER_GROUP * HEAD_LARGE), 1.0, 6.0, ((0, 8), (1, 4)))
    value_large = draw_value_large(jax.random.fold_in(key_list[19], 71), 0)
    key_bias = draw_key_bias(jax.random.fold_in(key_list[19], 71), 0)
    out_small = bell_draw(key_list[8], (HEADS_PER_GROUP * HEAD_SMALL, D), (HEADS_PER_GROUP * (HEAD_SMALL + HEAD_LARGE) // 48) ** -0.5, 0.75, ((0, 4),))
    out_large = bell_draw(key_list[9], (HEADS_PER_GROUP * HEAD_LARGE, D), (HEADS_PER_GROUP * (HEAD_SMALL + HEAD_LARGE) // 48) ** -0.5, 0.75, ((0, 4),))
    gain_one = jnp.clip(1.0 + 0.18 * jax.random.normal(key_list[10], (D,), jnp.float32), 0.1, 1.9)
    shift_one = bell_draw(key_list[11], (D,), 0.3, 1.5, (), jnp.float32)
    gain_two = jnp.clip(1.0 + 0.18 * jax.random.normal(key_list[12], (D,), jnp.float32), 0.1, 1.9)
    shift_two = bell_draw(key_list[13], (D,), 0.3, 1.5, (), jnp.float32)
    expert_pick = draw_expert_pick(jax.random.fold_in(key_list[19], 71), 0)
    route_weight = jnp.clip(0.2 + 0.8 * jax.random.uniform(key_list[15], (SEQUENCE_LENGTH, 2), jnp.float32) ** level_of(key_list[15], (SEQUENCE_LENGTH, 2), ((0, 8),), -0.2, 0.2), 0.2, 1.0)
    w_gate = bell_draw(key_list[16], (EXPERTS, D, FF_E), D ** -0.5, 0.125, ((0, 8), (2, 4)))
    w_up = bell_draw(key_list[17], (EXPERTS, D, FF_E), D ** -0.5, 0.125, ((0, 8), (2, 4)))
    w_down = bell_draw(key_list[18], (EXPERTS, FF_E, D), FF_E ** -0.5, 0.09375, ((0, 8), (1, 4)))
    return dict(stream=stream, query_small=query_small, key_small=key_small, value_small=value_small, query_large=query_large, key_large=key_large, value_large=value_large, key_bias=key_bias, out_small=out_small, out_large=out_large, gain_one=gain_one, shift_one=shift_one, gain_two=gain_two, shift_two=shift_two, expert_pick=expert_pick, route_weight=route_weight, w_gate=w_gate, w_up=w_up, w_down=w_down)


ALPHA_RES = 2.0 ** 0.25
NORM_EPS = 1e-05

def layer_norm(inputs, gain_vec, shift_vec):
    average = lax.optimization_barrier(jnp.mean(inputs, axis=-1, keepdims=True))
    centred = inputs - average
    variance = lax.optimization_barrier(jnp.mean(centred * centred, axis=-1, keepdims=True))
    return centred * lax.rsqrt(variance + NORM_EPS) * gain_vec + shift_vec

def stick_head(queries, key_rows, value_rows, log_bias):
    score_scale = queries.shape[1] ** (-0.5)
    outputs = []
    for block in range(SEQUENCE_LENGTH // TOK_DEV):
        first_row = block * TOK_DEV
        last_row = first_row + TOK_DEV
        scores = jnp.dot(queries[first_row:last_row], key_rows[:last_row].T, preferred_element_type=jnp.float32)
        scores = scores * score_scale + log_bias[:last_row].astype(jnp.float32)[None, :]
        query_pos = first_row + jnp.arange(TOK_DEV)
        key_pos = jnp.arange(last_row)
        causal = key_pos[None, :] < query_pos[:, None]
        log_stay = jnp.where(causal, jax.nn.log_sigmoid(-scores), 0.0)
        later_sum = lax.cumsum(log_stay, axis=1, reverse=True) - log_stay
        stick = jnp.where(causal, jnp.exp(jax.nn.log_sigmoid(scores) + later_sum), 0.0)
        outputs.append(jnp.dot(stick.astype(jnp.bfloat16), value_rows[:last_row], preferred_element_type=jnp.float32))
    return jnp.concatenate(outputs, 0).astype(jnp.bfloat16)

def stick_group(queries, key_rows, value_rows, log_bias):
    head_size = queries.shape[1] // HEADS_PER_GROUP

    def split_heads(array):
        return array.reshape(SEQUENCE_LENGTH, HEADS_PER_GROUP, head_size).transpose(1, 0, 2)

    def one_head(packed):
        return stick_head(packed[0], packed[1], packed[2], packed[3])
    outputs = lax.map(one_head, (split_heads(queries), split_heads(key_rows), split_heads(value_rows), log_bias.T))
    return outputs.transpose(1, 0, 2).reshape(SEQUENCE_LENGTH, HEADS_PER_GROUP * head_size)

def reference(stream, query_small, key_small, value_small, query_large, key_large, value_large, key_bias, out_small, out_large, gain_one, shift_one, gain_two, shift_two, expert_pick, route_weight, w_gate, w_up, w_down):
    att_small = stick_group(query_small, key_small, value_small, key_bias[:, 0, :])
    att_large = stick_group(query_large, key_large, value_large, key_bias[:, 1, :])
    run_heads = HEADS_PER_GROUP // N_TP
    small_cols = run_heads * HEAD_SMALL
    large_cols = run_heads * HEAD_LARGE
    mixer_out = jnp.zeros((SEQUENCE_LENGTH, D), jnp.float32)
    for shard_index in range(N_TP):
        term = jnp.dot(att_small[:, shard_index * small_cols:(shard_index + 1) * small_cols], out_small[shard_index * small_cols:(shard_index + 1) * small_cols], preferred_element_type=jnp.float32)
        term = term + jnp.dot(att_large[:, shard_index * large_cols:(shard_index + 1) * large_cols], out_large[shard_index * large_cols:(shard_index + 1) * large_cols], preferred_element_type=jnp.float32)
        mixer_out = mixer_out + lax.optimization_barrier(term.astype(jnp.bfloat16)).astype(jnp.float32)
    normed = layer_norm(ALPHA_RES * stream.astype(jnp.float32) + mixer_out, gain_one, shift_one).astype(jnp.bfloat16)
    blocks = SEQUENCE_LENGTH // TOK_DEV
    picks = expert_pick.reshape(blocks, TOK_DEV * 2)
    one_hot = (picks[:, :, None] == jnp.arange(EXPERTS)[None, None, :]).astype(jnp.int32)
    slot_rank = lax.optimization_barrier(jnp.sum((jnp.cumsum(one_hot, axis=1) - one_hot) * one_hot, axis=2)).astype(jnp.int32)
    block_ids = jnp.broadcast_to(jnp.arange(blocks, dtype=jnp.int32)[:, None], picks.shape)
    token_of = (jnp.arange(TOK_DEV * 2, dtype=jnp.int32) // 2)[None, :] + block_ids * TOK_DEV
    slot_table = jnp.zeros((EXPERTS, blocks, CAP), jnp.int32).at[picks, block_ids, slot_rank].set(token_of)
    width = FF_E // N_TP

    def expert_rows(packed):
        table, gate_w, up_w, down_w = packed
        rows_in = normed[table.reshape(-1)]
        gate = jnp.dot(rows_in, gate_w, preferred_element_type=jnp.float32)
        upper = jnp.dot(rows_in, up_w, preferred_element_type=jnp.float32)
        hidden = (jax.nn.silu(gate) * upper).astype(jnp.bfloat16)
        running = jnp.zeros((rows_in.shape[0], D), jnp.float32)
        for shard_index in range(N_TP):
            term = jnp.dot(hidden[:, shard_index * width:(shard_index + 1) * width], down_w[shard_index * width:(shard_index + 1) * width], preferred_element_type=jnp.float32)
            running = running + lax.optimization_barrier(term.astype(jnp.bfloat16)).astype(jnp.float32)
        return running.astype(jnp.bfloat16)
    results = lax.map(expert_rows, (slot_table, w_gate, w_up, w_down)).reshape(EXPERTS, blocks, CAP, D)
    chosen = results[picks, block_ids, slot_rank].reshape(SEQUENCE_LENGTH, 2, D).astype(jnp.float32)
    expert_mix = chosen[:, 0] * route_weight[:, 0:1] + chosen[:, 1] * route_weight[:, 1:2]
    return layer_norm(ALPHA_RES * normed.astype(jnp.float32) + expert_mix, gain_two, shift_two).astype(jnp.bfloat16)
```

```python
import functools

import jax
import jax.numpy as jnp
from jax import lax
from jax.experimental import pallas as pl
from jax.experimental.pallas import tpu as pltpu
from jax.sharding import PartitionSpec as P

HEAD_SMALL = 64
HEAD_LARGE = 128


ALPHA_RES = 2.0**0.25
NORM_EPS = 1e-05


def layer_norm(inputs, gain_vec, shift_vec):
    average = jnp.mean(inputs, axis=-1, keepdims=True)
    centred = inputs - average
    variance = jnp.mean(centred * centred, axis=-1, keepdims=True)
    return centred * lax.rsqrt(variance + NORM_EPS) * gain_vec + shift_vec


def stick_group(queries, key_rows, value_rows, log_bias, position):
    query_count = queries.shape[0]
    head_count = queries.shape[1]
    value_size = value_rows.shape[2]
    key_span = 4 * query_count
    score_scale = queries.shape[2] ** (-0.5)
    query_pos = position * query_count + jnp.arange(query_count, dtype=jnp.int32)
    block_count = (position * query_count + query_count + key_span - 1) // key_span

    def visit_block(turn_index, carry):
        running, stay_sum = carry
        first_key = (block_count - 1 - turn_index) * key_span
        key_block = lax.dynamic_slice_in_dim(key_rows, first_key, key_span, 0)
        value_block = lax.dynamic_slice_in_dim(value_rows, first_key, key_span, 0)
        bias_block = lax.dynamic_slice_in_dim(log_bias, first_key, key_span, 0).astype(jnp.float32)
        scores = jnp.einsum("qhd,khd->hqk", queries, key_block, preferred_element_type=jnp.float32)
        scores = scores * score_scale + bias_block.T[:, None, :]
        key_pos = first_key + jnp.arange(key_span, dtype=jnp.int32)
        causal = (key_pos[None, :] < query_pos[:, None])[None]
        log_stay = jnp.where(causal, jax.nn.log_sigmoid(-scores), 0.0)
        later_sum = lax.cumsum(log_stay, axis=2, reverse=True) - log_stay + stay_sum[:, :, None]
        stick_weight = jnp.where(
            causal, jnp.exp(jax.nn.log_sigmoid(scores) + later_sum), 0.0
        ).astype(jnp.bfloat16)
        running = running + jnp.einsum(
            "hqk,khd->qhd", stick_weight, value_block, preferred_element_type=jnp.float32
        )
        stay_sum = stay_sum + jnp.sum(log_stay, axis=2)
        return (running, stay_sum)

    start_total = jnp.zeros((query_count, head_count, value_size), jnp.float32)
    start_stay = jnp.zeros((head_count, query_count), jnp.float32)
    running, stay_sum = lax.fori_loop(0, block_count, visit_block, (start_total, start_stay))
    return running.reshape(query_count, head_count * value_size).astype(jnp.bfloat16)


def split_heads(array, head_size):
    return array.reshape(array.shape[0], array.shape[1] // head_size, head_size)


def local(
    stream,
    query_small,
    key_small,
    value_small,
    query_large,
    key_large,
    value_large,
    key_bias,
    out_small,
    out_large,
    gain_one,
    shift_one,
    gain_two,
    shift_two,
    expert_pick,
    route_weight,
    w_gate,
    w_up,
    w_down,
):
    row_count = stream.shape[0]
    position = lax.axis_index("sp")
    gathered = (
        lax.all_gather(key_small, "sp", axis=0, tiled=True),
        lax.all_gather(value_small, "sp", axis=0, tiled=True),
        lax.all_gather(key_large, "sp", axis=0, tiled=True),
        lax.all_gather(value_large, "sp", axis=0, tiled=True),
        lax.all_gather(key_bias, "sp", axis=0, tiled=True),
    )
    att_small = stick_group(
        split_heads(query_small, HEAD_SMALL),
        split_heads(gathered[0], HEAD_SMALL),
        split_heads(gathered[1], HEAD_SMALL),
        gathered[4][:, 0],
        position,
    )
    att_large = stick_group(
        split_heads(query_large, HEAD_LARGE),
        split_heads(gathered[2], HEAD_LARGE),
        split_heads(gathered[3], HEAD_LARGE),
        gathered[4][:, 1],
        position,
    )
    partial_value = jnp.dot(att_small, out_small, preferred_element_type=jnp.float32)
    partial_value = partial_value + jnp.dot(
        att_large, out_large, preferred_element_type=jnp.float32
    )
    mixer_out = lax.psum(partial_value.astype(jnp.bfloat16), "tp").astype(jnp.float32)
    normed = layer_norm(
        ALPHA_RES * stream.astype(jnp.float32) + mixer_out, gain_one, shift_one
    ).astype(jnp.bfloat16)
    experts = w_gate.shape[0] * lax.axis_size("sp")
    capacity = 4 * row_count // experts
    tp_count = lax.axis_size("tp")
    tp_index = lax.axis_index("tp")
    per_lane = capacity // tp_count
    flat_picks = expert_pick.reshape(-1)
    one_hot = (flat_picks[:, None] == jnp.arange(experts, dtype=jnp.int32)[None, :]).astype(
        jnp.int32
    )
    slot_rank = jnp.sum((jnp.cumsum(one_hot, axis=0) - one_hot) * one_hot, axis=1)
    slot_index = (flat_picks * capacity + slot_rank).reshape(row_count, 2)

    def selector(first_slot, slot_count):
        target = (
            jnp.arange(experts, dtype=jnp.int32)[:, None] * capacity
            + first_slot
            + jnp.arange(slot_count, dtype=jnp.int32)[None, :]
        ).reshape(-1)
        return [target[:, None] == slot_index[None, :, pick_index] for pick_index in range(2)]

    own_select = selector(tp_index * per_lane, per_lane)
    all_select = selector(0, capacity)
    placing = (all_select[0] | all_select[1]).astype(jnp.bfloat16)
    outgoing = jnp.dot(placing, normed, preferred_element_type=jnp.float32).astype(jnp.bfloat16)
    arrived = lax.all_to_all(
        outgoing.reshape(experts, capacity, normed.shape[1]),
        "sp",
        split_axis=0,
        concat_axis=0,
        tiled=True,
    )
    flat_rows = arrived.reshape(-1, arrived.shape[2])
    gate = jnp.dot(flat_rows, w_gate[0], preferred_element_type=jnp.float32)
    upper = jnp.dot(flat_rows, w_up[0], preferred_element_type=jnp.float32)
    hidden = (jax.nn.silu(gate) * upper).astype(jnp.bfloat16)
    expert_terms = jnp.dot(hidden, w_down[0], preferred_element_type=jnp.float32).reshape(
        arrived.shape
    )
    summed = lax.psum_scatter(
        expert_terms.astype(jnp.bfloat16), "tp", scatter_dimension=1, tiled=True
    )
    returned = lax.all_to_all(summed, "sp", split_axis=0, concat_axis=0, tiled=True).reshape(
        experts * per_lane, normed.shape[1]
    )
    picked_first = jnp.einsum(
        "sr,sd->rd",
        own_select[0].astype(jnp.bfloat16),
        returned,
        preferred_element_type=jnp.float32,
    )
    picked_second = jnp.einsum(
        "sr,sd->rd",
        own_select[1].astype(jnp.bfloat16),
        returned,
        preferred_element_type=jnp.float32,
    )
    partial_mix = route_weight[:, 0:1] * picked_first + route_weight[:, 1:2] * picked_second
    expert_mix = lax.psum_scatter(
        partial_mix.astype(jnp.bfloat16), "tp", scatter_dimension=0, tiled=True
    ).astype(jnp.float32)
    own_count = row_count // tp_count
    own_rows = lax.dynamic_slice_in_dim(normed, tp_index * own_count, own_count, 0).astype(
        jnp.float32
    )
    return layer_norm(ALPHA_RES * own_rows + expert_mix, gain_two, shift_two).astype(jnp.bfloat16)


GROUPS = 4


def fast_kernel(
    dims,
    qs_ref, ks_ref, vs_ref, ql_ref, kl_ref, vl_ref, bias_ref, stream_ref, os_ref, ol_ref,
    g1_ref, b1_ref, g2_ref, b2_ref, pick_ref, route_ref, wg_ref, wu_ref, wd_ref,
    out_ref,
    qs, ks, vs, ql, kl, vl, bias, g1, b1, g2, b2, pick, route,
    pack_a, pack_v, bias8, aq, ak, av, rb, tot, lat, ao, ra, wos, wol, strm, pb, rp, st, rst, normed,
    place, chosen, xs, wsend, wrecv, ag, xn, wg, wu, wd, acc, hid,
    y3, y2, y1, y0, dr, ts, rr, zs, zr, fs, fr,
    load_sem, q_send, q_recv, a_send, a_recv, p_send, p_recv, s_send, s_recv,
    x_send, x_recv, w_send, w_recv, g_send, g_recv, e_send, e_recv, d_send, d_recv,
    t_send, t_recv, z_send, z_recv, f_send, f_recv,
):
    n_sp, n_tp, rows, cols, cap, hs, hl = dims
    f32, bf16 = jnp.float32, jnp.bfloat16
    sp = lax.axis_index("sp")
    tp = lax.axis_index("tp")
    core = lax.rem(sp, 2)
    chip = lax.div(sp, 2)
    sibling = sp + 1 - 2 * core
    n_z = n_sp // 2
    is_small = core == 0
    ffw = wg_ref.shape[2]
    width = n_tp * cols

    def mesh_copy(src, dst, send, recv, target):
        return pltpu.make_async_remote_copy(
            src_ref=src, dst_ref=dst, send_sem=send, recv_sem=recv,
            device_id=target, device_id_type=pl.DeviceIdType.MESH,
        )

    def landed(ref, sem):
        pltpu.make_async_copy(ref, ref, sem).wait()

    def sp_at(j):
        return (j, tp)

    def tp_at(j):
        return (sp, j)

    def flip(index, mask, count):
        total, bit = 0, 1
        while bit < count:
            digit = lax.rem(lax.div(index, bit), 2)
            total = total + bit * (1 - digit if mask & bit else digit)
            bit *= 2
        return total

    z_order = [flip(chip, m, n_z) for m in range(n_z)]
    peers = [flip(tp, m, n_tp) for m in range(n_tp)]
    out_peers = [*peers[:0:-1], peers[0]]

    barrier = pltpu.get_barrier_semaphore()
    for k in range(1, n_sp):
        pl.semaphore_signal(barrier, inc=1, device_id=sp_at(lax.rem(sp + k, n_sp)), device_id_type=pl.DeviceIdType.MESH)
    for k in range(1, n_tp):
        pl.semaphore_signal(barrier, inc=1, device_id=tp_at(lax.rem(tp + k, n_tp)), device_id_type=pl.DeviceIdType.MESH)

    own_cols = pl.ds(pl.multiple_of(tp * cols, cols), cols)
    own_ff = pl.ds(pl.multiple_of(core * ffw, ffw), ffw)
    pairs = [
        (qs_ref, qs), (ks_ref, ks), (vs_ref, vs), (ql_ref, ql), (kl_ref, kl), (vl_ref, vl), (bias_ref, bias),
        (g1_ref, g1), (b1_ref, b1), (g2_ref, g2), (b2_ref, b2), (pick_ref, pick), (route_ref, route),
        (stream_ref.at[:, own_cols], strm), (os_ref, wos), (ol_ref, wol),
        (wg_ref.at[0], wg.at[core]), (wu_ref.at[0], wu.at[core]), (wd_ref.at[0], wd.at[own_ff]),
    ]
    loads = [pltpu.make_async_copy(src, dst, load_sem.at[n]) for n, (src, dst) in enumerate(pairs)]
    for load in loads[:13]:
        load.start()
    for load in loads[:7]:
        load.wait()

    for h in range(n_z):
        part = slice(h * hs, (h + 1) * hs)
        pack_a[h] = jnp.concatenate([qs[:, part], ks[:, part]], axis=1)
        pack_v[h] = jnp.concatenate([vs[:rows // 2, part], vs[rows // 2:, part]], axis=1)
        for kind in range(2):
            bias8[kind * n_z + h] = jnp.broadcast_to(bias[kind, h:h + 1, :].astype(f32), (8, rows))

    pl.semaphore_wait(barrier, n_sp + n_tp - 2)

    half_block = pl.ds(0, rows // 2)
    top = pl.ds(0, 1)

    def head_parts(kind, h, slot):
        if kind == 0:
            return [
                (0, pack_a.at[h], aq.at[slot]),
                (2, pack_v.at[h], av.at[slot, half_block]),
                (3, bias8.at[h, top], rb.at[slot, top]),
            ]
        part = pl.ds(pl.multiple_of(h * hl, hl), hl)
        return [
            (0, ql.at[:, part], aq.at[slot]),
            (1, kl.at[:, part], ak.at[slot]),
            (2, vl.at[:, part], av.at[slot]),
            (3, bias8.at[n_z + h, top], rb.at[slot, top]),
        ]

    def head_copies(z, kind):
        d = 2 * z + kind
        return [
            mesh_copy(src, dst, q_send.at[n, d], q_recv.at[n, sp], sp_at(d))
            for n, src, dst in head_parts(kind, z, sp)
        ]

    def for_targets(act):
        for kind in range(2):
            @pl.when(core != kind)
            def _():
                act(head_copies(chip, kind))
        for distance in range(1, n_z):
            for sign in (1, -1):
                z = chip + sign * distance

                @pl.when((z >= 0) & (z < n_z))
                def _():
                    for kind in range(2):
                        act(head_copies(z, kind))

    def start_all(copies):
        for copy in copies:
            copy.start()

    def sent_all(copies):
        for copy in copies:
            copy.wait_send()

    for_targets(start_all)
    for kind in range(2):
        @pl.when(core == kind)
        def _():
            for n, src, dst in head_parts(kind, chip, sp):
                pltpu.make_async_copy(src, dst, q_recv.at[n, sp]).start()

    for load in loads[13:]:
        load.start()
    weights = [
        mesh_copy(wg_ref.at[0], wg.at[core], e_send.at[0], e_recv.at[0], sp_at(sibling)),
        mesh_copy(wu_ref.at[0], wu.at[core], e_send.at[1], e_recv.at[1], sp_at(sibling)),
        mesh_copy(wd_ref.at[0], wd.at[own_ff], e_send.at[2], e_recv.at[2], sp_at(sibling)),
    ]
    start_all(weights)

    for load in loads[7:13]:
        load.wait()
    group = lax.div(pick[0:1, :], 2)
    first_even = lax.rem(pick[0:1, :], 2) == 0
    sub8 = lax.broadcasted_iota(jnp.int32, (8, rows), 0)
    one_hot = (sub8 == group).astype(f32)
    sub_r = lax.broadcasted_iota(jnp.int32, (rows, rows), 0)
    lane_r = lax.broadcasted_iota(jnp.int32, (rows, rows), 1)
    before = (sub_r < lane_r).astype(f32).astype(bf16)
    counts = jnp.dot(one_hot.astype(bf16), before, preferred_element_type=f32)
    rank = jnp.sum(one_hot * counts, axis=0, keepdims=True).astype(jnp.int32)
    slot_row = group * cap + rank
    slot_iota = lax.broadcasted_iota(jnp.int32, (GROUPS * cap, rows), 0)
    place[...] = (slot_iota == slot_row).astype(f32).astype(bf16)
    for g in range(GROUPS):
        chosen[g] = ((sub_r == slot_row - g * cap) & (sub_r < cap)).astype(f32).astype(bf16)

    def unfold(packed):
        tall = jnp.concatenate([packed[:, :hs], packed[:, hs:]], axis=0)
        return jnp.concatenate([tall, jnp.zeros_like(tall)], axis=1)

    lane_h = lax.broadcasted_iota(jnp.int32, (rows, hl), 1)

    def take(z):
        for half in range(2):
            j = 2 * z + half
            landed(rb.at[j, top], q_recv.at[3, j])
            landed(aq.at[j], q_recv.at[0, j])

            @pl.when(is_small)
            def _():
                folded = av.at[j, half_block]
                landed(folded, q_recv.at[2, j])
                both = aq[j]
                ak[j] = jnp.concatenate([both[:, hs:], both[:, :hs]], axis=1)
                aq[j] = jnp.where(lane_h < hs, both, jnp.zeros_like(both))
                av[j] = unfold(folded[...])

            @pl.when(jnp.logical_not(is_small))
            def _():
                landed(ak.at[j], q_recv.at[1, j])
                landed(av.at[j], q_recv.at[2, j])

    scale = jnp.where(is_small, hs**-0.5, hl**-0.5).astype(f32)
    span = 2 * rows
    sub_t = lax.broadcasted_iota(jnp.int32, (span, span), 0)
    lane_t = lax.broadcasted_iota(jnp.int32, (span, span), 1)
    tri = (sub_t >= lane_t).astype(f32).astype(bf16)
    causal = lane_t < sub_t

    def pair_of(ref, z):
        return ref[pl.ds(2 * z, 2)].reshape(span, hl)

    def tile(q, k, diagonal, later):
        log_odds = jnp.concatenate([rb[2 * k, 0:1, :], rb[2 * k + 1, 0:1, :]], axis=1)
        score = lax.dot_general(
            pair_of(aq, q), pair_of(ak, k), (((1,), (1,)), ((), ())), preferred_element_type=f32
        )
        score = score * scale + log_odds
        soft = jnp.maximum(score, 0.0) + jnp.log(1.0 + jnp.exp(-jnp.abs(score)))
        if diagonal:
            soft = jnp.where(causal, soft, 0.0)
        high = soft.astype(bf16)
        low = (soft - high.astype(f32)).astype(bf16)
        run = jnp.dot(high, tri, preferred_element_type=f32) + jnp.dot(low, tri, preferred_element_type=f32)
        if diagonal:
            stick = jnp.where(causal, jnp.exp(score - run), 0.0)
        else:
            stick = jnp.exp(score - run - later)
        added = jnp.dot(stick.astype(bf16), pair_of(av, k), preferred_element_type=f32)
        return added, run[:, 0:1]

    def head_back(d, small):
        src, dst = (ao.at[d, half_block], ra.at[sp, half_block]) if small else (ao.at[d], ra.at[sp])
        return src, dst, mesh_copy(src, dst, a_send.at[d], a_recv.at[sp], sp_at(d))

    def finish(q):
        for half in range(2):
            d = 2 * q + half
            block = tot[q, half * rows:(half + 1) * rows].astype(bf16)
            for small in (True, False):
                @pl.when(is_small if small else jnp.logical_not(is_small))
                def _():
                    if small:
                        ao[d, :rows // 2, :] = jnp.concatenate([block[:rows // 2, :hs], block[rows // 2:, :hs]], axis=1)
                    else:
                        ao[d] = block
                    src, dst, copy = head_back(d, small)

                    @pl.when(d != sp)
                    def _():
                        copy.start()

                    @pl.when(d == sp)
                    def _():
                        pltpu.make_async_copy(src, dst, a_recv.at[d]).start()

    lower = chip < n_z // 2
    mirrored = jnp.where(lower, chip, n_z - 1 - chip)
    for s in range(n_z):
        if s == 0:
            turn = mirrored
        elif s == 1:
            turn = 1 - mirrored
        else:
            turn = s
        z = jnp.where(lower, turn, n_z - 1 - turn)
        rising = lower if s != 1 else (lower == (mirrored == 0))
        take(z)
        added, current = tile(z, z, True, None)
        tot[z] = added
        lat[z] = current
        for i in range(1, s + 1):
            q = jnp.where(rising, z, z + i)
            k = jnp.where(rising, z - i, z)
            later = lat[q]
            added, current = tile(q, k, False, later)
            tot[q] = tot[q] + added
            lat[q] = later + current
        if s == 0:
            @pl.when(lower & (mirrored == 0))
            def _():
                finish(0)
        elif s == 1:
            @pl.when(lower & (mirrored == 1))
            def _():
                finish(0)

            @pl.when(lower)
            def _():
                finish(1)
        elif s < n_z - 1:
            @pl.when(lower)
            def _():
                finish(s)
        else:
            @pl.when(lower)
            def _():
                finish(s)

            @pl.when(jnp.logical_not(lower))
            def _():
                for q in range(n_z):
                    finish(q)

    for load in loads[13:16]:
        load.wait()
    for j in range(n_sp):
        landed(ra.at[j] if j % 2 else ra.at[j, half_block], a_recv.at[j])
    att_small = jnp.concatenate([unfold(ra[2 * h, :rows // 2, :])[:, :hs] for h in range(n_z)], axis=1)
    att_large = jnp.concatenate([ra[2 * h + 1] for h in range(n_z)], axis=1)

    for k in range(1, n_tp + 1):
        t = out_peers[k - 1]
        part = pl.ds(pl.multiple_of(t * cols, cols), cols)
        term = jnp.dot(att_small, wos[:, part], preferred_element_type=f32)
        term = term + jnp.dot(att_large, wol[:, part], preferred_element_type=f32)
        pb[k - 1] = term.astype(bf16)
        if k < n_tp:
            mesh_copy(pb.at[k - 1], rp.at[tp], p_send.at[k], p_recv.at[tp], tp_at(t)).start()
    mixed = ALPHA_RES * strm[...].astype(f32) + pb[n_tp - 1].astype(f32)
    for k in range(1, n_tp):
        landed(rp.at[peers[k]], p_recv.at[peers[k]])
        mixed = mixed + rp[peers[k]].astype(f32)

    eye = sub_r == lane_r

    def to_row(column):
        return jnp.sum(jnp.where(eye, column, 0.0), axis=0, keepdims=True)

    def to_column(row):
        return jnp.sum(jnp.where(eye, row, 0.0), axis=1, keepdims=True)

    own_mean = jnp.mean(mixed, axis=1, keepdims=True)
    centred = mixed - own_mean
    own_square = jnp.sum(centred * centred, axis=1, keepdims=True)
    mean_row, square_row = to_row(own_mean), to_row(own_square)
    st[...] = jnp.where(sub8 == 0, mean_row, square_row)
    for k in range(1, n_tp):
        mesh_copy(st, rst.at[tp], s_send.at[k], s_recv.at[tp], tp_at(peers[k])).start()

    sent = centred.astype(bf16)
    for g in range(GROUPS):
        xs[g] = jnp.dot(place[g * cap:(g + 1) * cap, :], sent, preferred_element_type=f32).astype(bf16)

    def x_copy(k):
        z = z_order[k]
        return mesh_copy(xs.at[z], ag.at[tp, chip], x_send.at[k], x_recv.at[chip], sp_at(2 * z + core))

    def g_copy(m, k):
        z = z_order[k]
        src = xs.at[chip] if k == 0 else ag.at[tp, z]
        return mesh_copy(src, ag.at[tp, z], g_send.at[m, z], g_recv.at[tp, z], tp_at(peers[m]))

    def g_relay(k):
        z = z_order[k]
        m = 1 if k < n_z // 2 else 2
        piece = ag.at[peers[m], z]
        return mesh_copy(piece, piece, g_send.at[3, z], g_recv.at[peers[m], z], tp_at(peers[3 - m]))

    def relay(k):
        m = 1 if k < n_z // 2 else 2
        landed(ag.at[peers[m], z_order[k]], g_recv.at[peers[m], z_order[k]])
        g_relay(k).start()

    for k in range(1, n_z):
        x_copy(k).start()
    pltpu.make_async_copy(xs.at[chip], ag.at[tp, chip], x_recv.at[chip]).start()
    for m in (1, 2):
        g_copy(m, 0).start()

    means, squares = [(tp, mean_row)], [square_row]
    for k in range(1, n_tp):
        src = peers[k]
        landed(rst.at[src], s_recv.at[src])
        means.append((src, rst[src, 0:1, :]))
        squares.append(rst[src, 1:2, :])
    full_mean = sum(m for _, m in means) / n_tp
    spread = sum(squares) + cols * sum((m - full_mean) * (m - full_mean) for _, m in means)
    scale_row = lax.rsqrt(spread / width + NORM_EPS)

    w_even = jnp.where(first_even, route[0:1, :], route[1:2, :])
    w_odd = jnp.where(first_even, route[1:2, :], route[0:1, :])
    w8 = jnp.where(sub8 == 0, w_even, jnp.where(sub8 == 1, w_odd, jnp.where(sub8 == 2, scale_row, 0.0)))
    for src, m in means:
        w8 = jnp.where(sub8 == 3 + src, m - full_mean, w8)
    w_hi = w8.astype(bf16)
    w_lo = (w8 - w_hi.astype(f32)).astype(bf16)
    last = (((1,), (1,)), ((), ()))
    for g in range(GROUPS):
        wsend[g] = lax.dot_general(w_hi, chosen[g], last, preferred_element_type=f32) + lax.dot_general(
            w_lo, chosen[g], last, preferred_element_type=f32
        )

    def w_copy(k):
        z = z_order[k]
        return mesh_copy(wsend.at[z], wrecv.at[chip], w_send.at[k], w_recv.at[chip], sp_at(2 * z + core))

    for k in range(1, n_z):
        w_copy(k).start()
    pltpu.make_async_copy(wsend.at[chip], wrecv.at[chip], w_recv.at[chip]).start()

    norm_val = (mixed - to_column(full_mean)) * to_column(scale_row) * g1[:, own_cols] + b1[:, own_cols]
    normed[...] = norm_val.astype(bf16)

    for k in range(n_z):
        landed(ag.at[tp, z_order[k]], x_recv.at[z_order[k]])
        if k:
            for m in (1, 2):
                g_copy(m, k).start()
        if k and k <= n_z // 2:
            relay(k - 1)
    for z in range(n_z):
        landed(wrecv.at[z], w_recv.at[z])
    for load in loads[16:]:
        load.wait()
    for copy in weights:
        copy.wait_recv()
    lane_c = lax.broadcasted_iota(jnp.int32, (cap, rows), 1)
    sub_c = lax.broadcasted_iota(jnp.int32, (cap, rows), 0)

    def slot_column(z, r):
        return jnp.sum(jnp.where(sub_c == lane_c, wrecv[z, pl.ds(r, 1), :], 0.0), axis=1, keepdims=True)

    rate = [slot_column(z, 2) for z in range(n_z)]
    slot_weight = [jnp.concatenate([slot_column(z, e) for z in range(n_z)], axis=0) for e in range(2)]
    step = min(512, ffw)

    def spread_in(m):
        t = peers[m]
        part = pl.ds(pl.multiple_of(t * cols, cols), cols)
        gain, shift = g1[:, part], b1[:, part]
        for z in range(n_z):
            value = (ag[t, z].astype(f32) + slot_column(z, 3 + t)) * rate[z] * gain + shift
            xn[z * cap:(z + 1) * cap, :] = value.astype(bf16)

    def up_half(m, e):
        inner = pl.ds(pl.multiple_of(peers[m] * cols, cols), cols)
        x = xn[...]
        for n in range(ffw // step):
            part = slice(n * step, (n + 1) * step)
            gate = jnp.dot(x, wg[e, inner, part], preferred_element_type=f32)
            upper = jnp.dot(x, wu[e, inner, part], preferred_element_type=f32)
            if m:
                gate = gate + acc[e, 0, :, part]
                upper = upper + acc[e, 1, :, part]
            if m < n_tp - 1:
                acc[e, 0, :, part] = gate
                acc[e, 1, :, part] = upper
            else:
                value = gate / (1.0 + jnp.exp(-gate)) * upper * slot_weight[e]
                hid[:, e * ffw + n * step:e * ffw + (n + 1) * step] = value.astype(bf16)

    def arrive(m, ks):
        for k in ks:
            landed(ag.at[peers[m], z_order[k]], g_recv.at[peers[m], z_order[k]])

    spread_in(0)
    up_half(0, 0)
    relay(2)
    up_half(0, 1)
    relay(3)
    arrive(1, (2, 3))
    spread_in(1)
    up_half(1, 0)
    up_half(1, 1)
    arrive(2, (0, 1))
    spread_in(2)
    up_half(2, 0)
    up_half(2, 1)
    arrive(3, range(n_z))
    spread_in(3)
    up_half(3, 0)
    up_half(3, 1)

    far, near = z_order[:1:-1], z_order[1::-1]

    def down(m):
        part = pl.ds(pl.multiple_of(peers[m] * cols, cols), cols)
        return jnp.dot(hid[...], wd[:, part], preferred_element_type=f32)

    def d_copy(m, z):
        return mesh_copy(y3.at[z], dr.at[m - 1, z], d_send.at[m - 1, z], d_recv.at[m - 1, z], tp_at(peers[m]))

    def t_copy(m, z):
        return mesh_copy(ts.at[m - 1, z], rr.at[m - 1, z], t_send.at[m - 1, z], t_recv.at[m - 1, z], tp_at(peers[m]))

    y3[...] = down(3).astype(bf16).reshape(n_z, cap, cols)
    for a, b in zip(far, near):
        d_copy(1, a).start()
        d_copy(2, b).start()
    y2[...] = down(2).reshape(n_z, cap, cols)
    for z in near:
        ts[1, z] = y2[z].astype(bf16)
        t_copy(2, z).start()
    y1[...] = down(1).reshape(n_z, cap, cols)
    for z in far:
        ts[0, z] = y1[z].astype(bf16)
        t_copy(1, z).start()
    y0[...] = down(0).reshape(n_z, cap, cols)
    for a, b in zip(far, near):
        landed(dr.at[0, a], d_recv.at[0, a])
        ts[1, a] = (y2[a] + dr[0, a].astype(f32)).astype(bf16)
        t_copy(2, a).start()
        landed(dr.at[1, b], d_recv.at[1, b])
        ts[0, b] = (y1[b] + dr[1, b].astype(f32)).astype(bf16)
        t_copy(1, b).start()

    def z_copy(z):
        return mesh_copy(zs.at[z], zr.at[chip], z_send.at[z], z_recv.at[chip], sp_at(2 * z + core))

    for k, z in enumerate([*far, *near]):
        for m in range(2):
            landed(rr.at[m, z], t_recv.at[m, z])
        zs[z] = (y0[z] + rr[0, z].astype(f32) + rr[1, z].astype(f32)).astype(bf16)
        if k < n_z - 1:
            z_copy(z).start()
        else:
            pltpu.make_async_copy(zs.at[z], zr.at[chip], z_recv.at[chip]).start()
    for z in range(n_z):
        landed(zr.at[z], z_recv.at[z])
    expert_mix = lax.dot_general(
        place[...], zr[...].reshape(n_z * cap, cols), (((0,), (0,)), ((), ())), preferred_element_type=f32
    )
    final = ALPHA_RES * normed[...].astype(f32) + expert_mix
    own_rows = rows // n_tp
    middle = jnp.mean(final, axis=1, keepdims=True)
    middle_hi = middle.astype(bf16)
    middle_lo = (middle - middle_hi.astype(f32)).astype(bf16)
    packed = (final - (middle_hi.astype(f32) + middle_lo.astype(f32))).astype(bf16)
    extra = jnp.where(lane_h < hs, middle_hi.astype(f32), middle_lo.astype(f32)).astype(bf16)
    for t in range(n_tp):
        fs[t, :, :cols] = packed[t * own_rows:(t + 1) * own_rows]
        fs[t, :, cols:] = extra[t * own_rows:(t + 1) * own_rows]

    def f_copy(k):
        return mesh_copy(fs.at[peers[k]], fr.at[tp], f_send.at[k], f_recv.at[tp], tp_at(peers[k]))

    for k in range(n_tp - 1, 0, -1):
        f_copy(k).start()
    pltpu.make_async_copy(fs.at[tp], fr.at[tp], f_recv.at[tp]).start()
    for t in range(n_tp):
        landed(fr.at[t], f_recv.at[t])
    blocks = []
    for t in range(n_tp):
        tail = fr[t, :, cols:].astype(f32)
        blocks.append(fr[t, :, :cols].astype(f32) + (tail[:, 0:1] + tail[:, hs:hs + 1]))
    average = sum(jnp.sum(b, axis=1, keepdims=True) for b in blocks) / width
    blocks = [b - average for b in blocks]
    variance = sum(jnp.sum(b * b, axis=1, keepdims=True) for b in blocks) / width
    inverse = lax.rsqrt(variance + NORM_EPS)
    for t in range(n_tp):
        part = slice(t * cols, (t + 1) * cols)
        out_ref[:, part] = (blocks[t] * inverse * g2[:, part] + b2[:, part]).astype(bf16)

    for_targets(sent_all)
    sent_all(weights)
    for d in range(n_sp):
        for small in (True, False):
            @pl.when((d != sp) & (is_small if small else jnp.logical_not(is_small)))
            def _():
                head_back(d, small)[2].wait_send()
    for k in range(1, n_tp):
        mesh_copy(pb.at[k - 1], rp.at[tp], p_send.at[k], p_recv.at[tp], tp_at(out_peers[k - 1])).wait_send()
        mesh_copy(st, rst.at[tp], s_send.at[k], s_recv.at[tp], tp_at(peers[k])).wait_send()
        f_copy(k).wait_send()
    for k in range(1, n_z):
        x_copy(k).wait_send()
        w_copy(k).wait_send()
    for k in range(n_z):
        g_copy(1, k).wait_send()
        g_copy(2, k).wait_send()
        g_relay(k).wait_send()
    for a, b in zip(far, near):
        d_copy(1, a).wait_send()
        d_copy(2, b).wait_send()
    for z in z_order:
        t_copy(1, z).wait_send()
        t_copy(2, z).wait_send()
    for z in z_order[1:]:
        z_copy(z).wait_send()


def fast_local(
    stream, query_small, key_small, value_small, query_large, key_large, value_large, key_bias,
    out_small, out_large, gain_one, shift_one, gain_two, shift_two, expert_pick, route_weight,
    w_gate, w_up, w_down,
):
    f32, bf16 = jnp.float32, jnp.bfloat16
    n_sp, n_tp = lax.axis_size("sp"), lax.axis_size("tp")
    rows, width = stream.shape
    cols = width // n_tp
    hs, hl = HEAD_SMALL, HEAD_LARGE
    cap = 4 * rows // (w_gate.shape[0] * n_sp)
    n_z = n_sp // 2
    ffw = w_gate.shape[2]
    hbm = pl.BlockSpec(memory_space=pl.ANY)
    dma = pltpu.SemaphoreType.DMA
    V = pltpu.VMEM
    slots = n_z * cap
    operands = (
        query_small, key_small, value_small, query_large, key_large, value_large,
        key_bias.transpose(1, 2, 0), stream, out_small, out_large,
        gain_one[None], shift_one[None], gain_two[None], shift_two[None],
        expert_pick.T, route_weight.T, w_gate, w_up, w_down,
    )
    kept = [*operands[:7], *operands[10:16]]
    scratch = [
        *[V(a.shape, a.dtype) for a in kept],
        V((n_z, rows, hl), bf16), V((n_z, rows // 2, hl), bf16), V((n_sp, 8, rows), f32),
        V((n_sp, rows, hl), bf16), V((n_sp, rows, hl), bf16), V((n_sp, rows, hl), bf16),
        V((n_sp, 8, rows), f32),
        V((n_z, 2 * rows, hl), f32), V((n_z, 2 * rows, 1), f32),
        V((n_sp, rows, hl), bf16), V((n_sp, rows, hl), bf16),
        V(out_small.shape, bf16), V(out_large.shape, bf16), V((rows, cols), bf16),
        V((n_tp, rows, cols), bf16), V((n_tp, rows, cols), bf16),
        V((8, rows), f32), V((n_tp, 8, rows), f32), V((rows, cols), bf16),
        V((GROUPS * cap, rows), bf16), V((GROUPS, rows, rows), bf16), V((GROUPS, cap, cols), bf16),
        V((GROUPS, 8, rows), f32), V((n_z, 8, rows), f32),
        V((n_tp, n_z, cap, cols), bf16), V((slots, cols), bf16),
        V((2, width, ffw), bf16), V((2, width, ffw), bf16), V((2 * ffw, width), bf16),
        V((2, 2, slots, ffw), f32), V((slots, 2 * ffw), bf16),
        V((n_z, cap, cols), bf16), V((n_z, cap, cols), f32), V((n_z, cap, cols), f32), V((n_z, cap, cols), f32),
        V((2, n_z, cap, cols), bf16), V((2, n_z, cap, cols), bf16), V((2, n_z, cap, cols), bf16),
        V((n_z, cap, cols), bf16), V((n_z, cap, cols), bf16),
        V((n_tp, rows // n_tp, cols + hl), bf16), V((n_tp, rows // n_tp, cols + hl), bf16),
        dma((19,)), dma((4, n_sp)), dma((4, n_sp)), dma((n_sp,)), dma((n_sp,)),
        dma((n_tp,)), dma((n_tp,)), dma((n_tp,)), dma((n_tp,)),
        dma((n_z,)), dma((n_z,)), dma((n_z,)), dma((n_z,)),
        dma((n_tp, n_z)), dma((n_tp, n_z)), dma((3,)), dma((3,)),
        dma((2, n_z)), dma((2, n_z)), dma((2, n_z)), dma((2, n_z)),
        dma((n_z,)), dma((n_z,)), dma((n_tp,)), dma((n_tp,)),
    ]
    dims = (n_sp, n_tp, rows, cols, cap, hs, hl)
    return pl.pallas_call(
        functools.partial(fast_kernel, dims),
        out_shape=jax.ShapeDtypeStruct((rows // n_tp, width), bf16),
        in_specs=[hbm] * len(operands),
        out_specs=pl.BlockSpec(memory_space=pltpu.VMEM),
        scratch_shapes=scratch,
        compiler_params=pltpu.CompilerParams(
            collective_id=0, has_side_effects=True, vmem_limit_bytes=60 * 1024 * 1024
        ),
        name="layer",
    )(*operands)


def layer(*arrays):
    n_sp, n_tp = lax.axis_size("sp"), lax.axis_size("tp")
    rows, width = arrays[0].shape
    small, large = arrays[1].shape[1] // HEAD_SMALL, arrays[4].shape[1] // HEAD_LARGE
    experts = arrays[16].shape[0] * n_sp
    paired = experts == 2 * GROUPS and n_sp == experts and n_tp == GROUPS
    if paired and small == large and 2 * small == n_sp and rows == HEAD_LARGE and width % (128 * n_tp) == 0:
        return fast_local(*arrays)
    return local(*arrays)


def solution(mesh):
    placed = (
        P("sp", None),
        P("sp", "tp"),
        P("sp", "tp"),
        P("sp", "tp"),
        P("sp", "tp"),
        P("sp", "tp"),
        P("sp", "tp"),
        P("sp", None, "tp"),
        P("tp", None),
        P("tp", None),
        P(),
        P(),
        P(),
        P(),
        P("sp", None),
        P("sp", None),
        P("sp", None, "tp"),
        P("sp", None, "tp"),
        P("sp", "tp", None),
    )
    return jax.shard_map(
        layer, mesh=mesh, in_specs=placed, out_specs=P(("sp", "tp"), None), check_vma=False
    )
```
